32 devices in a mesh: sp: 16 (over z, y, x), tp: 2 (over core).
Axes of the slice: x: 2, y: 2, z: 4, core: 2. Of those that a mesh axis runs over, the one named last changes fastest.
Arguments:
- queries: bfloat16 [2048, 1024], P('sp', 'tp'), may hold values from -6 to 6
- attn_out: bfloat16 [2048, 1024], P('sp', 'tp'), may hold values from -6 to 6
- out_grad: bfloat16 [2048, 1024], P('sp', 'tp'), may hold values from -384 to 384
- row_lse: float32 [2048, 8], P('sp', 'tp'), may hold values from 9.5 to 12.5
- source: bfloat16 [8192, 4096], P('sp', 'tp'), may hold values from -6 to 6
- saved_keys: bfloat16 [8192, 256], P('sp'), may hold values from -6 to 6
- saved_values: bfloat16 [8192, 256], P('sp'), may hold values from -6 to 6
- key_weight: bfloat16 [4096, 256], P('tp'), may hold values from -0.09375 to 0.09375
- value_weight: bfloat16 [4096, 256], P('tp'), may hold values from -0.09375 to 0.09375
Outputs:
- query_grad: float32 [2048, 1024], P('sp', 'tp')
- source_grad: float32 [8192, 4096], P('sp', 'tp')
- key_grad: float32 [256, 4096], P('sp', 'tp')
The draws below stay inside these ranges and needn't reach their ends.
All inputs are finite; a program needn't handle non-finite values.
Results may differ from the reference program's by a relative error of at most 0.012.
Values may be sent and summed in bfloat16 or wider, within the bound.
A program may use at most 64 MiB of HBM per device.

```python
import math
import jax
import jax.numpy as jnp
from jax import lax

D = 4096
HEADS = 8
KV_HEADS = 2
HEAD_DIM = 128
TARGET_ROWS = 2048
SOURCE_ROWS = 8192


def levels(rng, extent, cuts, smallest, largest):
    def one(position, parts):
        heights = jax.random.uniform(jax.random.fold_in(jax.random.fold_in(rng, 6), position), (parts,), jnp.float32, smallest / len(cuts), largest / len(cuts))
        return jnp.repeat(jnp.exp(heights), extent[position] // parts).reshape((-1,) + (1,) * (len(extent) - position - 1))

    gain = one(*cuts[0])
    for cut in cuts[1:]:
        gain = gain * one(*cut)
    return gain


def normal_values(rng, dims, deviation, reach, pieces=(), dtype=jnp.bfloat16):
    array = deviation * jax.random.normal(rng, dims, jnp.float32)
    if pieces:
        array = array * levels(rng, dims, pieces, -0.22, 0.18)
    return jnp.clip(array, -reach, reach).astype(dtype)


def setup_inputs(seed: int = 0) -> dict:
    arg_keys = jax.random.split(jax.random.key(seed), 10)
    return {
        "queries": normal_values(arg_keys[0], (TARGET_ROWS, HEADS * HEAD_DIM), 1.0, 6.0, ((0, 16), (1, 2))),
        "attn_out": normal_values(arg_keys[1], (TARGET_ROWS, HEADS * HEAD_DIM), 1.0, 6.0, ((0, 16), (1, 2))),
        "out_grad": normal_values(arg_keys[2], (TARGET_ROWS, HEADS * HEAD_DIM), 64.0, 384.0, ((0, 16), (1, 2))),
        "row_lse": jnp.clip(9.5 + 3.0 * jax.random.uniform(arg_keys[3], (TARGET_ROWS, HEADS), jnp.float32) ** levels(arg_keys[3], (TARGET_ROWS, HEADS), ((0, 16), (1, 2)), -0.2, 0.2), 9.5, 12.5),
        "source": normal_values(arg_keys[4], (SOURCE_ROWS, D), 1.0, 6.0, ((0, 16), (1, 2))),
        "saved_keys": normal_values(arg_keys[5], (SOURCE_ROWS, KV_HEADS * HEAD_DIM), 1.0, 6.0, ((0, 16),)),
        "saved_values": normal_values(arg_keys[6], (SOURCE_ROWS, KV_HEADS * HEAD_DIM), 1.0, 6.0, ((0, 16),)),
        "key_weight": normal_values(arg_keys[7], (D, KV_HEADS * HEAD_DIM), D ** -0.5, 0.09375, ((0, 2),)),
        "value_weight": normal_values(arg_keys[8], (D, KV_HEADS * HEAD_DIM), D ** -0.5, 0.09375, ((0, 2),)),
    }


def reference(queries, attn_out, out_grad, row_lse, source, saved_keys, saved_values, key_weight, value_weight):
    per_key = HEADS // KV_HEADS
    score_scale = 1.0 / math.sqrt(HEAD_DIM)
    tgt_len = queries.shape[0]
    src_len = source.shape[0]
    span = math.gcd(tgt_len, 1024)
    count = tgt_len // span
    row_delta = lax.optimization_barrier(jnp.sum((out_grad.astype(jnp.float32) * attn_out.astype(jnp.float32)).reshape(-1, HEADS, HEAD_DIM), axis=2))
    key_acc = jnp.zeros((src_len, KV_HEADS * HEAD_DIM), jnp.float32)
    value_acc = jnp.zeros((src_len, KV_HEADS * HEAD_DIM), jnp.float32)
    head_parts = []
    for head_index in range(HEADS):
        kv_lo = head_index // per_key * HEAD_DIM
        col_lo = head_index * HEAD_DIM
        key_head = saved_keys[:, kv_lo:kv_lo + HEAD_DIM]
        value_head = saved_values[:, kv_lo:kv_lo + HEAD_DIM]
        query_blocks = queries[:, col_lo:col_lo + HEAD_DIM].reshape(count, span, HEAD_DIM)
        grad_blocks = out_grad[:, col_lo:col_lo + HEAD_DIM].reshape(count, span, HEAD_DIM)
        lse_blocks = row_lse[:, head_index:head_index + 1].reshape(count, span, 1)
        delta_blocks = row_delta[:, head_index:head_index + 1].reshape(count, span, 1)

        def step(carry, items):
            key_part, value_part = carry
            query_head, grad_head, lse_col, delta_col = items
            scores = jnp.dot(query_head, key_head.T, preferred_element_type=jnp.float32) * score_scale
            attn_probs = jnp.exp(scores - lse_col)
            dprobs = jnp.dot(grad_head, value_head.T, preferred_element_type=jnp.float32)
            dscores = (attn_probs * (dprobs - delta_col) * score_scale).astype(jnp.bfloat16)
            key_part = key_part + jnp.dot(dscores.T, query_head, preferred_element_type=jnp.float32)
            value_part = value_part + jnp.dot(attn_probs.astype(jnp.bfloat16).T, grad_head, preferred_element_type=jnp.float32)
            return ((key_part, value_part), jnp.dot(dscores, key_head, preferred_element_type=jnp.float32))
        empty = jnp.zeros((src_len, HEAD_DIM), jnp.float32)
        (key_part, value_part), query_blocks_out = lax.scan(step, (empty, empty), (query_blocks, grad_blocks, lse_blocks, delta_blocks))
        head_parts.append(query_blocks_out.reshape(tgt_len, HEAD_DIM))
        key_acc = key_acc.at[:, kv_lo:kv_lo + HEAD_DIM].add(key_part)
        value_acc = value_acc.at[:, kv_lo:kv_lo + HEAD_DIM].add(value_part)
    query_grad = jnp.concatenate(head_parts, axis=1)
    key_half = key_acc.astype(jnp.bfloat16)
    value_half = value_acc.astype(jnp.bfloat16)
    source_grad = jnp.dot(key_half, key_weight.T, preferred_element_type=jnp.float32) + jnp.dot(value_half, value_weight.T, preferred_element_type=jnp.float32)
    key_grad = jnp.dot(key_half.T, source, preferred_element_type=jnp.float32) * (1.0 / math.sqrt(source.shape[0]))
    return (query_grad, source_grad, key_grad)
```

```python
import functools
import math

import jax
import jax.numpy as jnp
from jax import lax
from jax.experimental import pallas as pl
from jax.experimental.pallas import tpu as pltpu
from jax.sharding import PartitionSpec as P

HEADS = 8
KV_HEADS = 2
HEAD_DIM = 128
LOG2E = 1.0 / math.log(2.0)
MESH = pl.DeviceIdType.MESH
F32 = jnp.float32
BF16 = jnp.bfloat16


def dot_nt(left, right, precision=None):
    return lax.dot_general(
        left, right, (((1,), (1,)), ((), ())), preferred_element_type=F32, precision=precision
    )


def dot_tn(left, right):
    return lax.dot_general(left, right, (((0,), (0,)), ((), ())), preferred_element_type=F32)


def dot_nn(left, right):
    return jnp.dot(left, right, preferred_element_type=F32)


def kernel(
    tgt_n, src_n, tp_n, src_total,
    q_ref, o_ref, d_ref, lse_ref, key_ref, value_ref, source_ref,
    dq_ref, kv_ref, kg_ref,
    qd, stats, kvs, dk, dv, dq_acc, dq_own, dq_out, dq_in, g_out, g_in, tp_own, tp_in,
    src, w_own, w_out, w_in, w2_out, w2_in,
    copy_sem, qd_s, qd_r, st_s, st_r, kv_s, kv_r, dq_s, dq_r, g_s, g_r, tp_s, tp_r,
    w_s, w_r, w2_s, w2_r,
):
    sp = lax.axis_index("sp")
    tp = lax.axis_index("tp")
    me_t, me_s = sp // src_n, sp % src_n
    rows = q_ref.shape[0]
    heads = q_ref.shape[1] // HEAD_DIM
    src_rows = key_ref.shape[0]
    per_key = HEADS // KV_HEADS
    scale = 1.0 / math.sqrt(HEAD_DIM)
    kv_col = pl.multiple_of(tp * heads // per_key * HEAD_DIM, HEAD_DIM)
    t_peers = [lax.rem(me_t + k, tgt_n) for k in range(1, tgt_n)]
    s_peers = [lax.rem(me_s + k, src_n) for k in range(1, src_n)]
    tp_peers = [lax.rem(tp + k, tp_n) for k in range(1, tp_n)]

    def t_dev(t):
        return {"sp": t * src_n + me_s, "tp": tp}

    def s_dev(s):
        return {"sp": me_t * src_n + s, "tp": tp}

    def tp_dev(p):
        return {"sp": sp, "tp": p}

    def remote(source, target, send, recv, device):
        return pltpu.make_async_remote_copy(
            src_ref=source, dst_ref=target, send_sem=send, recv_sem=recv,
            device_id=device, device_id_type=MESH,
        )

    load = pltpu.make_async_copy(source_ref, src, copy_sem)
    load.start()
    barrier = pltpu.get_barrier_semaphore()
    for t in t_peers:
        pl.semaphore_signal(barrier, inc=1, device_id=t_dev(t), device_id_type=MESH)
    for s in s_peers:
        pl.semaphore_signal(barrier, inc=1, device_id=s_dev(s), device_id_type=MESH)
    for p in tp_peers:
        pl.semaphore_signal(barrier, inc=1, device_id=tp_dev(p), device_id_type=MESH)
    pl.semaphore_wait(barrier, tgt_n + src_n + tp_n - 3)

    for t in t_peers:
        for h in range(heads):
            for i, ref in enumerate((q_ref, d_ref)):
                remote(
                    ref.at[:, pl.ds(h * HEAD_DIM, HEAD_DIM)],
                    qd.at[me_t, i, pl.ds(h * rows, rows), :],
                    qd_s.at[t], qd_r.at[me_t], t_dev(t),
                ).start()
    for s in s_peers:
        for i, ref in enumerate((key_ref, value_ref)):
            remote(
                ref.at[:, pl.ds(kv_col, HEAD_DIM)], kvs.at[me_s, i],
                kv_s.at[s], kv_r.at[me_s], s_dev(s),
            ).start()

    ones = jnp.ones((8, HEAD_DIM), F32)
    for h in range(heads):
        cols = pl.ds(h * HEAD_DIM, HEAD_DIM)
        span = pl.ds(h * rows, rows)
        prod = d_ref[:, cols].astype(F32) * o_ref[:, cols].astype(F32)
        delta = dot_nt(ones, prod, lax.Precision.HIGHEST)
        stats[me_t, 0:1, span] = lse_ref[h : h + 1, :] * LOG2E
        stats[me_t, 1:2, span] = delta[0:1, :]
        qd[me_t, 0, span, :] = q_ref[:, cols]
        qd[me_t, 1, span, :] = d_ref[:, cols]
    kvs[me_s, 0] = key_ref[:, pl.ds(kv_col, HEAD_DIM)]
    kvs[me_s, 1] = value_ref[:, pl.ds(kv_col, HEAD_DIM)]
    dk[...] = jnp.zeros_like(dk)
    dv[...] = jnp.zeros_like(dv)
    for t in t_peers:
        remote(stats.at[me_t], stats.at[me_t], st_s.at[t], st_r.at[me_t], t_dev(t)).start()

    def tile(t, s):
        q, d = qd[t, 0], qd[t, 1]
        k, v = kvs[s, 0], kvs[s, 1]
        scores = dot_nt(k, q)
        probs = jnp.exp2(scores * (scale * LOG2E) - stats[t, 0:1, :])
        dprobs = dot_nt(v, d)
        dscores = (probs * (dprobs - stats[t, 1:2, :])).astype(BF16)
        dv[s] += dot_nn(probs.astype(BF16), d)
        dk[s] += dot_nn(dscores, q)
        dq_acc[...] += dot_tn(dscores, k)

    def send_dq(t):
        dq_out[t] = (dq_acc[...] * scale).astype(BF16)
        remote(dq_out.at[t], dq_in.at[me_t], dq_s.at[t], dq_r.at[me_t], t_dev(t)).start()

    def send_kv(s):
        g_out[s, 0] = (dk[s] * scale).astype(BF16)
        g_out[s, 1] = dv[s].astype(BF16)
        remote(g_out.at[s], g_in.at[me_s], g_s.at[s], g_r.at[me_s], s_dev(s)).start()

    dq_acc[...] = jnp.zeros_like(dq_acc)
    tile(me_t, me_s)
    for s in s_peers:
        remote(kvs.at[s], kvs.at[s], kv_s.at[s], kv_r.at[s], s_dev(s)).wait_recv()
        tile(me_t, s)
    dq_own[...] = dq_acc[...] * scale
    for n, t in enumerate(t_peers):
        remote(qd.at[t], qd.at[t], qd_s.at[t], qd_r.at[t], t_dev(t)).wait_recv()
        remote(stats.at[t], stats.at[t], st_s.at[t], st_r.at[t], t_dev(t)).wait_recv()
        dq_acc[...] = jnp.zeros_like(dq_acc)
        if n < tgt_n - 2:

            def body(s, carry, t=t):
                tile(t, s)
                return carry

            lax.fori_loop(0, src_n, body, 0)
        else:
            for s in s_peers:
                tile(t, s)
                send_kv(s)
            tile(t, me_s)
        send_dq(t)

    dk_total = dk[me_s] * scale
    dv_total = dv[me_s]
    for s in s_peers:
        remote(g_in.at[s], g_in.at[s], g_s.at[s], g_r.at[s], s_dev(s)).wait_recv()
        dk_total += g_in[s, 0].astype(F32)
        dv_total += g_in[s, 1].astype(F32)
    tp_own[0] = dk_total.astype(BF16)
    tp_own[1] = dv_total.astype(BF16)
    for p in tp_peers:
        remote(tp_own, tp_in.at[tp], tp_s.at[p], tp_r.at[tp], tp_dev(p)).start()
    tp_in[tp] = tp_own[...]
    for p in tp_peers:
        remote(tp_in.at[p], tp_in.at[p], tp_s.at[p], tp_r.at[p], tp_dev(p)).wait_recv()
    for i in range(2):
        for g in range(KV_HEADS):
            owners = [p for p in range(tp_n) if p * heads // per_key == g]
            half = tp_in[owners[0], i]
            if len(owners) > 1:
                total = half.astype(F32)
                for p in owners[1:]:
                    total += tp_in[p, i].astype(F32)
                half = total.astype(BF16)
            kv_ref[:, pl.ds((i * KV_HEADS + g) * HEAD_DIM, HEAD_DIM)] = half

    load.wait()
    part = w_own.shape[1]
    key_half = kv_ref[:, 0 : KV_HEADS * HEAD_DIM]
    w_scale = 1.0 / math.sqrt(src_total)
    partial = dot_tn(key_half, src[...]) * w_scale
    for t in range(tgt_n):
        for s in range(src_n):
            low = (t * src_n + s) * part
            w_out[s, t] = partial[low : low + part].astype(BF16)
    for s in s_peers:
        remote(w_out.at[s], w_in.at[me_s], w_s.at[s], w_r.at[me_s], s_dev(s)).start()

    dq_total = dq_own[...]
    for t in t_peers:
        remote(dq_in.at[t], dq_in.at[t], dq_s.at[t], dq_r.at[t], t_dev(t)).wait_recv()
        dq_total += dq_in[t].astype(F32)
    for h in range(heads):
        dq_ref[:, h * HEAD_DIM : (h + 1) * HEAD_DIM] = dq_total[h * rows : (h + 1) * rows]

    w_total = w_out[me_s].astype(F32)
    for s in s_peers:
        remote(w_in.at[s], w_in.at[s], w_s.at[s], w_r.at[s], s_dev(s)).wait_recv()
        w_total += w_in[s].astype(F32)
    w_own[...] = w_total
    w2_out[...] = w_total.astype(BF16)
    for t in t_peers:
        remote(w2_out.at[t], w2_in.at[me_t], w2_s.at[t], w2_r.at[me_t], t_dev(t)).start()
    kg_total = w_own[me_t]
    for t in t_peers:
        remote(w2_in.at[t], w2_in.at[t], w2_s.at[t], w2_r.at[t], t_dev(t)).wait_recv()
        kg_total += w2_in[t].astype(F32)
    kg_ref[...] = kg_total

    for t in t_peers:
        remote(qd.at[t], qd.at[t], qd_s.at[t], qd_r.at[t], t_dev(t)).wait_send()
        remote(stats.at[t], stats.at[t], st_s.at[t], st_r.at[t], t_dev(t)).wait_send()
        remote(dq_out.at[t], dq_in.at[t], dq_s.at[t], dq_r.at[t], t_dev(t)).wait_send()
        remote(w2_out.at[t], w2_in.at[t], w2_s.at[t], w2_r.at[t], t_dev(t)).wait_send()
    for s in s_peers:
        remote(kvs.at[s], kvs.at[s], kv_s.at[s], kv_r.at[s], s_dev(s)).wait_send()
        remote(g_out.at[s], g_in.at[s], g_s.at[s], g_r.at[s], s_dev(s)).wait_send()
        remote(w_out.at[s], w_in.at[s], w_s.at[s], w_r.at[s], s_dev(s)).wait_send()
    for p in tp_peers:
        remote(tp_own, tp_in.at[p], tp_s.at[p], tp_r.at[p], tp_dev(p)).wait_send()


def shards(
    tgt_n, src_n, tp_n,
    queries, attn_out, out_grad, row_lse, source, saved_keys, saved_values, key_weight, value_weight
):
    heads = row_lse.shape[1]
    rows, width = queries.shape
    src_rows, columns = source.shape
    kv_width = KV_HEADS * HEAD_DIM
    sp_n = tgt_n * src_n
    part = kv_width // sp_n
    stacked = heads * rows
    dma = pltpu.SemaphoreType.DMA
    vmem = pl.BlockSpec(memory_space=pltpu.VMEM)
    scratch = [
        pltpu.VMEM((tgt_n, 2, stacked, HEAD_DIM), BF16),
        pltpu.VMEM((tgt_n, 8, stacked), F32),
        pltpu.VMEM((src_n, 2, src_rows, HEAD_DIM), BF16),
        pltpu.VMEM((src_n, src_rows, HEAD_DIM), F32),
        pltpu.VMEM((src_n, src_rows, HEAD_DIM), F32),
        pltpu.VMEM((stacked, HEAD_DIM), F32),
        pltpu.VMEM((stacked, HEAD_DIM), F32),
        pltpu.VMEM((tgt_n, stacked, HEAD_DIM), BF16),
        pltpu.VMEM((tgt_n, stacked, HEAD_DIM), BF16),
        pltpu.VMEM((src_n, 2, src_rows, HEAD_DIM), BF16),
        pltpu.VMEM((src_n, 2, src_rows, HEAD_DIM), BF16),
        pltpu.VMEM((2, src_rows, HEAD_DIM), BF16),
        pltpu.VMEM((tp_n, 2, src_rows, HEAD_DIM), BF16),
        pltpu.VMEM((src_rows, columns), BF16),
        pltpu.VMEM((tgt_n, part, columns), F32),
        pltpu.VMEM((src_n, tgt_n, part, columns), BF16),
        pltpu.VMEM((src_n, tgt_n, part, columns), BF16),
        pltpu.VMEM((tgt_n, part, columns), BF16),
        pltpu.VMEM((tgt_n, part, columns), BF16),
        dma,
    ]
    for count in (tgt_n, tgt_n, src_n, tgt_n, src_n, tp_n, src_n, tgt_n):
        scratch += [dma((count,)), dma((count,))]
    query_grad, kv_half, key_grad = pl.pallas_call(
        functools.partial(kernel, tgt_n, src_n, tp_n, src_rows * sp_n),
        out_shape=(
            jax.ShapeDtypeStruct((rows, width), F32),
            jax.ShapeDtypeStruct((src_rows, 2 * kv_width), BF16),
            jax.ShapeDtypeStruct((part, columns), F32),
        ),
        in_specs=[vmem] * 6 + [pl.BlockSpec(memory_space=pl.ANY)],
        out_specs=(vmem, vmem, vmem),
        scratch_shapes=scratch,
        compiler_params=pltpu.CompilerParams(
            collective_id=0, has_side_effects=True, vmem_limit_bytes=60 * 2**20
        ),
        name="attention_grads",
    )(queries, attn_out, out_grad, row_lse.T, saved_keys, saved_values, source)
    source_grad = dot_nt(kv_half[:, :kv_width], key_weight) + dot_nt(
        kv_half[:, kv_width:], value_weight
    )
    return (query_grad, source_grad, key_grad)


def solution(mesh):
    sp_n, tp_n = mesh.shape["sp"], mesh.shape["tp"]
    src_n = 2 ** (int(math.log2(sp_n)) // 2)
    in_specs = (
        P("sp", "tp"),
        P("sp", "tp"),
        P("sp", "tp"),
        P("sp", "tp"),
        P("sp", "tp"),
        P("sp", None),
        P("sp", None),
        P("tp", None),
        P("tp", None),
    )
    out_specs = (P("sp", "tp"), P("sp", "tp"), P("sp", "tp"))
    return jax.shard_map(
        functools.partial(shards, sp_n // src_n, src_n, tp_n),
        mesh=mesh, in_specs=in_specs, out_specs=out_specs, check_vma=False,
    )
```

```python
import functools
import math

import jax
import jax.numpy as jnp
from jax import lax
from jax.experimental import pallas as pl
from jax.experimental.pallas import tpu as pltpu
from jax.sharding import PartitionSpec as P

HEADS = 8
KV_HEADS = 2
HEAD_DIM = 128
LOG2E = 1.0 / math.log(2.0)
MESH = pl.DeviceIdType.MESH
F32 = jnp.float32
BF16 = jnp.bfloat16


def dot_nt(left, right, precision=None):
    return lax.dot_general(
        left, right, (((1,), (1,)), ((), ())), preferred_element_type=F32, precision=precision
    )


def dot_tn(left, right):
    return lax.dot_general(left, right, (((0,), (0,)), ((), ())), preferred_element_type=F32)


def dot_nn(left, right):
    return jnp.dot(left, right, preferred_element_type=F32)


def kernel(
    tgt_n, src_n, key_n, tp_n, src_total,
    q_ref, o_ref, d_ref, lse_ref, key_ref, value_ref, source_ref,
    dq_ref, kv_ref, kg_ref,
    qd, stats, kvs, dk, dv, dq_acc, dq_out, dq_in, g_out, g_in, tp_own, tp_in,
    src, a_out, a_in, a2_own, a2_out, a2_in, b_out, b_in, b2_own, b2_out, b2_in,
    copy_sem, qd_s, qd_r, rq_s, st_s, st_r, kv_s, kv_r, rkv_s, dq_s, dq_r, g_s, g_r, tp_s, tp_r,
    a_s, a_r, a2_s, a2_r, b_s, b_r, b2_s, b2_r,
):
    sp = lax.axis_index("sp")
    tp = lax.axis_index("tp")
    sp_n = tgt_n * src_n
    t_hi, t_lo = sp // (2 * src_n), sp % 2
    me_t = t_hi * 2 + t_lo
    me_s = (sp // 2) % src_n
    s_hi, s_lo = me_s // 2, me_s % 2
    near_t, near_s = t_hi * 2 + 1 - t_lo, s_hi * 2 + 1 - s_lo
    t_his = [lax.rem(t_hi + k, tgt_n // 2) for k in range(1, tgt_n // 2)]
    s_his = [lax.rem(s_hi + k, src_n // 2) for k in range(1, src_n // 2)]
    far_t = [hi * 2 + t_lo for hi in t_his]
    diag_t = [hi * 2 + 1 - t_lo for hi in t_his]
    far_s = [hi * 2 + s_lo for hi in s_his]
    diag_s = [hi * 2 + 1 - s_lo for hi in s_his]
    t_peers = far_t + [near_t] + diag_t
    s_peers = far_s + [near_s] + diag_s
    key_m = sp_n // key_n
    me_o, me_i = sp // key_n, sp % key_n
    o_peers = [lax.rem(me_o + k, key_m) for k in range(1, key_m)]
    i_peers = [lax.rem(me_i + k, key_n) for k in range(1, key_n)]
    tp_peers = [lax.rem(tp + k, tp_n) for k in range(1, tp_n)]
    rows = q_ref.shape[0]
    heads = q_ref.shape[1] // HEAD_DIM
    chunks = qd.shape[1]
    per_chunk = heads // chunks
    src_rows = key_ref.shape[0]
    per_key = HEADS // KV_HEADS
    scale = 1.0 / math.sqrt(HEAD_DIM)
    kv_col = pl.multiple_of(tp * heads // per_key * HEAD_DIM, HEAD_DIM)

    def t_dev(t):
        return {"sp": t // 2 * (2 * src_n) + me_s * 2 + t % 2, "tp": tp}

    def s_dev(s):
        return {"sp": t_hi * (2 * src_n) + s * 2 + t_lo, "tp": tp}

    def o_dev(o):
        return {"sp": o * key_n + me_i, "tp": tp}

    def i_dev(i):
        return {"sp": me_o * key_n + i, "tp": tp}

    def tp_dev(p):
        return {"sp": sp, "tp": p}

    def remote(source, target, send, recv, device):
        return pltpu.make_async_remote_copy(
            src_ref=source, dst_ref=target, send_sem=send, recv_sem=recv,
            device_id=device, device_id_type=MESH,
        )

    load = pltpu.make_async_copy(source_ref, src, copy_sem)
    load.start()
    barrier = pltpu.get_barrier_semaphore()
    for k in range(1, sp_n):
        pl.semaphore_signal(
            barrier, inc=1, device_id={"sp": lax.rem(sp + k, sp_n), "tp": tp}, device_id_type=MESH
        )
    for p in tp_peers:
        pl.semaphore_signal(barrier, inc=1, device_id=tp_dev(p), device_id_type=MESH)
    pl.semaphore_wait(barrier, sp_n + tp_n - 2)

    def send_q(t):
        for c in range(chunks):
            for h in range(per_chunk):
                for i, ref in enumerate((q_ref, d_ref)):
                    remote(
                        ref.at[:, pl.ds((c * per_chunk + h) * HEAD_DIM, HEAD_DIM)],
                        qd.at[me_t, c, i, pl.ds(h * rows, rows), :],
                        qd_s.at[t, c], qd_r.at[me_t, c], t_dev(t),
                    ).start()

    for s in far_s + [near_s]:
        for i, ref in enumerate((key_ref, value_ref)):
            remote(
                ref.at[:, pl.ds(kv_col, HEAD_DIM)], kvs.at[me_s, i],
                kv_s.at[s], kv_r.at[me_s], s_dev(s),
            ).start()
    for t in far_t + [near_t]:
        send_q(t)

    ones = jnp.ones((8, HEAD_DIM), F32)
    for h in range(heads):
        cols = pl.ds(h * HEAD_DIM, HEAD_DIM)
        c, span = h // per_chunk, pl.ds(h % per_chunk * rows, rows)
        prod = d_ref[:, cols].astype(F32) * o_ref[:, cols].astype(F32)
        delta = dot_nt(ones, prod, lax.Precision.HIGHEST)
        stats[me_t, c, 0:1, span] = lse_ref[h : h + 1, :] * LOG2E
        stats[me_t, c, 1:2, span] = delta[0:1, :]
        qd[me_t, c, 0, span, :] = q_ref[:, cols]
        qd[me_t, c, 1, span, :] = d_ref[:, cols]
    kvs[me_s, 0] = key_ref[:, pl.ds(kv_col, HEAD_DIM)]
    kvs[me_s, 1] = value_ref[:, pl.ds(kv_col, HEAD_DIM)]
    dk[...] = jnp.zeros_like(dk)
    dv[...] = jnp.zeros_like(dv)
    dq_acc[...] = jnp.zeros_like(dq_acc)
    for t in t_peers:
        remote(stats.at[me_t], stats.at[me_t], st_s.at[t], st_r.at[me_t], t_dev(t)).start()

    def tile(t, s):
        def body(c, carry):
            q, d = qd[t, c, 0], qd[t, c, 1]
            k, v = kvs[s, 0], kvs[s, 1]
            scores = dot_nt(k, q)
            probs = jnp.exp2(scores * (scale * LOG2E) - stats[t, c, 0:1, :])
            dprobs = dot_nt(v, d)
            dscores = (probs * (dprobs - stats[t, c, 1:2, :])).astype(BF16)
            dv[s] += dot_nn(probs.astype(BF16), d)
            dk[s] += dot_nn(dscores, q)
            dq_acc[t, c] += dot_tn(dscores, k)
            return carry

        lax.fori_loop(0, chunks, body, 0)

    def got_q(t, c):
        remote(qd.at[t, c], qd.at[t, c], qd_s.at[t, c], qd_r.at[t, c], t_dev(t)).wait_recv()

    def got_stats(t):
        remote(stats.at[t], stats.at[t], st_s.at[t], st_r.at[t], t_dev(t)).wait_recv()

    def got_kv(s):
        remote(kvs.at[s], kvs.at[s], kv_s.at[s], kv_r.at[s], s_dev(s)).wait_recv()

    def relay_q(t, c):
        return remote(
            qd.at[t, c], qd.at[t, c], rq_s.at[t, c], qd_r.at[t, c], t_dev(near_t)
        )

    def relay_kv(s):
        return remote(kvs.at[s], kvs.at[s], rkv_s.at[s], kv_r.at[s], s_dev(near_s))

    def send_dq(t):
        dq_out[t] = (dq_acc[t] * scale).astype(BF16)
        remote(dq_out.at[t], dq_in.at[me_t], dq_s.at[t], dq_r.at[me_t], t_dev(t)).start()

    def send_g(s, i):
        g_out[s, i] = dv[s].astype(BF16) if i else (dk[s] * scale).astype(BF16)
        remote(
            g_out.at[s, i], g_in.at[me_s, i], g_s.at[s, i], g_r.at[me_s, i], s_dev(s)
        ).start()

    tile(me_t, me_s)
    for s in far_s:
        got_kv(s)
        relay_kv(s).start()
    got_kv(near_s)
    tile(me_t, near_s)
    for c in range(chunks):
        for t in far_t:
            got_q(t, c)
            relay_q(t, c).start()
        if c == 0:
            for s in far_s:
                tile(me_t, s)
            for c2 in range(chunks):
                got_q(near_t, c2)
            got_stats(near_t)
    for s in [me_s, near_s] + far_s:
        tile(near_t, s)
    for t in far_t:
        got_stats(t)
        for s in [me_s, near_s] + far_s:
            tile(t, s)
    for s in diag_s:
        got_kv(s)
        for t in [near_t] + far_t + [me_t]:
            tile(t, s)
    for t in [near_t] + far_t:
        send_dq(t)
    for n, t in enumerate(diag_t):
        for c in range(chunks):
            got_q(t, c)
        got_stats(t)
        for s in far_s + diag_s + [near_s]:
            tile(t, s)
            if n == len(diag_t) - 1:
                send_g(s, 0)
        if n == len(diag_t) - 1:
            for s in far_s + diag_s + [near_s]:
                send_g(s, 1)
        tile(t, me_s)
        send_dq(t)

    def reduce_g(i):
        total = dv[me_s] if i else dk[me_s] * scale
        for s in s_peers:
            remote(
                g_in.at[s, i], g_in.at[s, i], g_s.at[s, i], g_r.at[s, i], s_dev(s)
            ).wait_recv()
            total += g_in[s, i].astype(F32)
        tp_own[i] = total.astype(BF16)
        for p in tp_peers:
            remote(
                tp_own.at[i], tp_in.at[tp, i], tp_s.at[p, i], tp_r.at[tp, i], tp_dev(p)
            ).start()
        tp_in[tp, i] = tp_own[i]

    def gather_g(i):
        for p in tp_peers:
            remote(
                tp_in.at[p, i], tp_in.at[p, i], tp_s.at[p, i], tp_r.at[p, i], tp_dev(p)
            ).wait_recv()
        for g in range(KV_HEADS):
            owners = [p for p in range(tp_n) if p * heads // per_key == g]
            half = tp_in[owners[0], i]
            if len(owners) > 1:
                total = half.astype(F32)
                for p in owners[1:]:
                    total += tp_in[p, i].astype(F32)
                half = total.astype(BF16)
            kv_ref[:, pl.ds((i * KV_HEADS + g) * HEAD_DIM, HEAD_DIM)] = half

    reduce_g(0)
    load.wait()
    gather_g(0)
    part = a2_own.shape[1]
    cut = a2_own.shape[2]
    key_half = kv_ref[:, 0 : KV_HEADS * HEAD_DIM]
    w_scale = 1.0 / math.sqrt(src_total)
    partial = dot_tn(key_half, src[...]) * w_scale
    for o in range(key_m):
        for i in range(key_n):
            low = (o * key_n + i) * part
            block = partial[low : low + part].astype(BF16)
            a_out[i, o] = block[:, :cut]
            b_out[o, i] = block[:, cut:]
    for i in i_peers:
        remote(a_out.at[i], a_in.at[me_i], a_s.at[i], a_r.at[me_i], i_dev(i)).start()
    for o in o_peers:
        remote(b_out.at[o], b_in.at[me_o], b_s.at[o], b_r.at[me_o], o_dev(o)).start()

    reduce_g(1)
    gather_g(1)
    dq_total = dq_acc[me_t] * scale
    for t in t_peers:
        remote(dq_in.at[t], dq_in.at[t], dq_s.at[t], dq_r.at[t], t_dev(t)).wait_recv()
        dq_total += dq_in[t].astype(F32)
    for h in range(heads):
        low = h % per_chunk * rows
        dq_ref[:, h * HEAD_DIM : (h + 1) * HEAD_DIM] = dq_total[h // per_chunk, low : low + rows]

    total = b_out[me_o].astype(F32)
    for o in o_peers:
        remote(b_in.at[o], b_in.at[o], b_s.at[o], b_r.at[o], o_dev(o)).wait_recv()
        total += b_in[o].astype(F32)
    b2_own[...] = total
    b2_out[...] = total.astype(BF16)
    for i in i_peers:
        remote(b2_out.at[i], b2_in.at[me_i], b2_s.at[i], b2_r.at[me_i], i_dev(i)).start()
    total = a_out[me_i].astype(F32)
    for i in i_peers:
        remote(a_in.at[i], a_in.at[i], a_s.at[i], a_r.at[i], i_dev(i)).wait_recv()
        total += a_in[i].astype(F32)
    a2_own[...] = total
    a2_out[...] = total.astype(BF16)
    for o in o_peers:
        remote(a2_out.at[o], a2_in.at[me_o], a2_s.at[o], a2_r.at[me_o], o_dev(o)).start()
    total = b2_own[me_i]
    for i in i_peers:
        remote(b2_in.at[i], b2_in.at[i], b2_s.at[i], b2_r.at[i], i_dev(i)).wait_recv()
        total += b2_in[i].astype(F32)
    kg_ref[:, cut:] = total
    total = a2_own[me_o]
    for o in o_peers:
        remote(a2_in.at[o], a2_in.at[o], a2_s.at[o], a2_r.at[o], o_dev(o)).wait_recv()
        total += a2_in[o].astype(F32)
    kg_ref[:, :cut] = total

    for t in far_t + [near_t]:
        for c in range(chunks):
            remote(qd.at[t, c], qd.at[t, c], qd_s.at[t, c], qd_r.at[t, c], t_dev(t)).wait_send()
    for t in far_t:
        for c in range(chunks):
            relay_q(t, c).wait_send()
    for t in t_peers:
        remote(stats.at[t], stats.at[t], st_s.at[t], st_r.at[t], t_dev(t)).wait_send()
        remote(dq_out.at[t], dq_in.at[t], dq_s.at[t], dq_r.at[t], t_dev(t)).wait_send()
    for s in far_s + [near_s]:
        remote(kvs.at[s], kvs.at[s], kv_s.at[s], kv_r.at[s], s_dev(s)).wait_send()
    for s in far_s:
        relay_kv(s).wait_send()
    for s in s_peers:
        for i in range(2):
            remote(
                g_out.at[s, i], g_in.at[s, i], g_s.at[s, i], g_r.at[s, i], s_dev(s)
            ).wait_send()
    for i in i_peers:
        remote(a_out.at[i], a_in.at[i], a_s.at[i], a_r.at[i], i_dev(i)).wait_send()
        remote(b2_out.at[i], b2_in.at[i], b2_s.at[i], b2_r.at[i], i_dev(i)).wait_send()
    for o in o_peers:
        remote(b_out.at[o], b_in.at[o], b_s.at[o], b_r.at[o], o_dev(o)).wait_send()
        remote(a2_out.at[o], a2_in.at[o], a2_s.at[o], a2_r.at[o], o_dev(o)).wait_send()
    for p in tp_peers:
        for i in range(2):
            remote(
                tp_own.at[i], tp_in.at[p, i], tp_s.at[p, i], tp_r.at[p, i], tp_dev(p)
            ).wait_send()


def shards(
    tgt_n, src_n, tp_n,
    queries, attn_out, out_grad, row_lse, source, saved_keys, saved_values, key_weight, value_weight
):
    heads = row_lse.shape[1]
    rows, width = queries.shape
    src_rows, columns = source.shape
    kv_width = KV_HEADS * HEAD_DIM
    sp_n = tgt_n * src_n
    part = kv_width // sp_n
    key_n, key_m = src_n, tgt_n
    chunks = math.gcd(heads, 2)
    stacked = heads // chunks * rows
    cut = (2 * columns // 3 + 127) // 128 * 128
    rest = columns - cut
    dma = pltpu.SemaphoreType.DMA
    vmem = pl.BlockSpec(memory_space=pltpu.VMEM)
    scratch = [
        pltpu.VMEM((tgt_n, chunks, 2, stacked, HEAD_DIM), BF16),
        pltpu.VMEM((tgt_n, chunks, 8, stacked), F32),
        pltpu.VMEM((src_n, 2, src_rows, HEAD_DIM), BF16),
        pltpu.VMEM((src_n, src_rows, HEAD_DIM), F32),
        pltpu.VMEM((src_n, src_rows, HEAD_DIM), F32),
        pltpu.VMEM((tgt_n, chunks, stacked, HEAD_DIM), F32),
        pltpu.VMEM((tgt_n, chunks, stacked, HEAD_DIM), BF16),
        pltpu.VMEM((tgt_n, chunks, stacked, HEAD_DIM), BF16),
        pltpu.VMEM((src_n, 2, src_rows, HEAD_DIM), BF16),
        pltpu.VMEM((src_n, 2, src_rows, HEAD_DIM), BF16),
        pltpu.VMEM((2, src_rows, HEAD_DIM), BF16),
        pltpu.VMEM((tp_n, 2, src_rows, HEAD_DIM), BF16),
        pltpu.VMEM((src_rows, columns), BF16),
        pltpu.VMEM((key_n, key_m, part, cut), BF16),
        pltpu.VMEM((key_n, key_m, part, cut), BF16),
        pltpu.VMEM((key_m, part, cut), F32),
        pltpu.VMEM((key_m, part, cut), BF16),
        pltpu.VMEM((key_m, part, cut), BF16),
        pltpu.VMEM((key_m, key_n, part, rest), BF16),
        pltpu.VMEM((key_m, key_n, part, rest), BF16),
        pltpu.VMEM((key_n, part, rest), F32),
        pltpu.VMEM((key_n, part, rest), BF16),
        pltpu.VMEM((key_n, part, rest), BF16),
        dma,
    ]
    for shape in (
        (tgt_n, chunks), (tgt_n, chunks), (tgt_n, chunks), (tgt_n,), (tgt_n,),
        (src_n,), (src_n,), (src_n,), (tgt_n,), (tgt_n,), (src_n, 2), (src_n, 2),
        (tp_n, 2), (tp_n, 2), (key_n,), (key_n,), (key_m,), (key_m,),
        (key_m,), (key_m,), (key_n,), (key_n,),
    ):
        scratch.append(dma(shape))
    query_grad, kv_half, key_grad = pl.pallas_call(
        functools.partial(kernel, tgt_n, src_n, key_n, tp_n, src_rows * sp_n),
        out_shape=(
            jax.ShapeDtypeStruct((rows, width), F32),
            jax.ShapeDtypeStruct((src_rows, 2 * kv_width), BF16),
            jax.ShapeDtypeStruct((part, columns), F32),
        ),
        in_specs=[vmem] * 6 + [pl.BlockSpec(memory_space=pl.ANY)],
        out_specs=(vmem, vmem, vmem),
        scratch_shapes=scratch,
        compiler_params=pltpu.CompilerParams(
            collective_id=0, has_side_effects=True, vmem_limit_bytes=60 * 2**20
        ),
        name="attention_grads",
    )(queries, attn_out, out_grad, row_lse.T, saved_keys, saved_values, source)
    source_grad = dot_nt(kv_half[:, :kv_width], key_weight) + dot_nt(
        kv_half[:, kv_width:], value_weight
    )
    return (query_grad, source_grad, key_grad)


def solution(mesh):
    sp_n, tp_n = mesh.shape["sp"], mesh.shape["tp"]
    src_n = 2 ** (int(math.log2(sp_n)) // 2)
    in_specs = (
        P("sp", "tp"),
        P("sp", "tp"),
        P("sp", "tp"),
        P("sp", "tp"),
        P("sp", "tp"),
        P("sp", None),
        P("sp", None),
        P("tp", None),
        P("tp", None),
    )
    out_specs = (P("sp", "tp"), P("sp", "tp"), P("sp", "tp"))
    return jax.shard_map(
        functools.partial(shards, sp_n // src_n, src_n, tp_n),
        mesh=mesh, in_specs=in_specs, out_specs=out_specs, check_vma=False,
    )
```

```python
import functools
import math

import jax
import jax.numpy as jnp
from jax import lax
from jax.experimental import pallas as pl
from jax.experimental.pallas import tpu as pltpu
from jax.sharding import PartitionSpec as P

HEADS = 8
KV_HEADS = 2
HEAD_DIM = 128
LOG2E = 1.0 / math.log(2.0)
MESH = pl.DeviceIdType.MESH
F32 = jnp.float32
BF16 = jnp.bfloat16


def dot_nt(left, right, precision=None):
    return lax.dot_general(
        left, right, (((1,), (1,)), ((), ())), preferred_element_type=F32, precision=precision
    )


def dot_tn(left, right):
    return lax.dot_general(left, right, (((0,), (0,)), ((), ())), preferred_element_type=F32)


def dot_nn(left, right):
    return jnp.dot(left, right, preferred_element_type=F32)


def kernel(
    tgt_n, src_n, key_n, tp_n, src_total,
    q_ref, o_ref, d_ref, lse_ref, key_ref, value_ref, source_ref,
    dq_ref, kv_ref, kg_ref,
    qd, stats, kvs, dk, dv, dq_acc, dq_out, dq_in, dq_via, g_out, g_in, tp_own, tp_in,
    src, a_out, a_in, a2_own, a2_out, a2_in, b_out, b_in, b2_own, b2_out, b2_in,
    copy_sem, qd_s, qd_r, rq_s, st_s, st_r, kv_s, kv_r, rkv_s, dq_s, dq_r, via_r, g_s, g_r, tp_s, tp_r,
    a_s, a_r, a2_s, a2_r, b_s, b_r, b2_s, b2_r,
):
    sp = lax.axis_index("sp")
    tp = lax.axis_index("tp")
    sp_n = tgt_n * src_n
    t_hi, t_lo = sp // (2 * src_n), sp % 2
    me_t = t_hi * 2 + t_lo
    me_s = (sp // 2) % src_n
    s_hi, s_lo = me_s // 2, me_s % 2
    near_t, near_s = t_hi * 2 + 1 - t_lo, s_hi * 2 + 1 - s_lo
    t_his = [lax.rem(t_hi + k, tgt_n // 2) for k in range(1, tgt_n // 2)]
    s_his = [lax.rem(s_hi + k, src_n // 2) for k in range(1, src_n // 2)]
    far_t = [hi * 2 + t_lo for hi in t_his]
    diag_t = [hi * 2 + 1 - t_lo for hi in t_his]
    far_s = [hi * 2 + s_lo for hi in s_his]
    diag_s = [hi * 2 + 1 - s_lo for hi in s_his]
    t_peers = far_t + [near_t] + diag_t
    s_peers = far_s + [near_s] + diag_s
    key_m = sp_n // key_n
    me_o, me_i = sp // key_n, sp % key_n
    o_peers = [lax.rem(me_o + k, key_m) for k in range(1, key_m)]
    i_peers = [lax.rem(me_i + k, key_n) for k in range(1, key_n)]
    tp_peers = [lax.rem(tp + k, tp_n) for k in range(1, tp_n)]
    rows = q_ref.shape[0]
    heads = q_ref.shape[1] // HEAD_DIM
    chunks = stats.shape[1]
    per_chunk = heads // chunks
    src_rows = key_ref.shape[0]
    per_key = HEADS // KV_HEADS
    scale = 1.0 / math.sqrt(HEAD_DIM)
    kv_col = pl.multiple_of(tp * heads // per_key * HEAD_DIM, HEAD_DIM)

    def t_dev(t):
        return {"sp": t // 2 * (2 * src_n) + me_s * 2 + t % 2, "tp": tp}

    def s_dev(s):
        return {"sp": t_hi * (2 * src_n) + s * 2 + t_lo, "tp": tp}

    def o_dev(o):
        return {"sp": o * key_n + me_i, "tp": tp}

    def i_dev(i):
        return {"sp": me_o * key_n + i, "tp": tp}

    def tp_dev(p):
        return {"sp": sp, "tp": p}

    def remote(source, target, send, recv, device):
        return pltpu.make_async_remote_copy(
            src_ref=source, dst_ref=target, send_sem=send, recv_sem=recv,
            device_id=device, device_id_type=MESH,
        )

    load = pltpu.make_async_copy(source_ref, src, copy_sem)
    load.start()
    barrier = pltpu.get_barrier_semaphore()
    for k in range(1, sp_n):
        pl.semaphore_signal(
            barrier, inc=1, device_id={"sp": lax.rem(sp + k, sp_n), "tp": tp}, device_id_type=MESH
        )
    for p in tp_peers:
        pl.semaphore_signal(barrier, inc=1, device_id=tp_dev(p), device_id_type=MESH)
    ones = jnp.ones((8, HEAD_DIM), F32)
    for h in range(heads):
        cols = pl.ds(h * HEAD_DIM, HEAD_DIM)
        c, span = h // per_chunk, pl.ds(h % per_chunk * rows, rows)
        prod = d_ref[:, cols].astype(F32) * o_ref[:, cols].astype(F32)
        delta = dot_nt(ones, prod, lax.Precision.HIGHEST)
        stats[me_t, c, 0:1, span] = lse_ref[h : h + 1, :] * LOG2E
        stats[me_t, c, 1:2, span] = delta[0:1, :]
    kvs[me_s, 0] = key_ref[:, pl.ds(kv_col, HEAD_DIM)]
    kvs[me_s, 1] = value_ref[:, pl.ds(kv_col, HEAD_DIM)]
    qd[me_t, 0] = q_ref[...]
    qd[me_t, 1] = d_ref[...]
    dk[...] = jnp.zeros_like(dk)
    dv[...] = jnp.zeros_like(dv)
    dq_acc[...] = jnp.zeros_like(dq_acc)
    pl.semaphore_wait(barrier, sp_n + tp_n - 2)

    def send_q(t):
        for i, ref in enumerate((q_ref, d_ref)):
            remote(ref, qd.at[me_t, i], qd_s.at[t, i], qd_r.at[me_t, i], t_dev(t)).start()

    for s in far_s + [near_s]:
        remote(kvs.at[me_s], kvs.at[me_s], kv_s.at[s], kv_r.at[me_s], s_dev(s)).start()
    for t in far_t + [near_t]:
        send_q(t)

    for t in t_peers:
        remote(stats.at[me_t], stats.at[me_t], st_s.at[t], st_r.at[me_t], t_dev(t)).start()

    def stack(t, i, c):
        low = c * per_chunk
        return jnp.concatenate(
            [
                qd[t, i, :, pl.ds(pl.multiple_of((low + h) * HEAD_DIM, HEAD_DIM), HEAD_DIM)]
                for h in range(per_chunk)
            ],
            axis=0,
        )

    def tile(t, s):
        def body(c, carry):
            q, d = stack(t, 0, c), stack(t, 1, c)
            k, v = kvs[s, 0], kvs[s, 1]
            scores = dot_nt(k, q)
            probs = jnp.exp2(scores * (scale * LOG2E) - stats[t, c, 0:1, :])
            dprobs = dot_nt(v, d)
            dscores = (probs * (dprobs - stats[t, c, 1:2, :])).astype(BF16)
            dv[s] += dot_nn(probs.astype(BF16), d)
            dk[s] += dot_nn(dscores, q)
            dq_acc[t, c] += dot_tn(dscores, k)
            return carry

        lax.fori_loop(0, chunks, body, 0)

    def got_q(t, c):
        remote(qd.at[t, c], qd.at[t, c], qd_s.at[t, c], qd_r.at[t, c], t_dev(t)).wait_recv()

    def got_stats(t):
        remote(stats.at[t], stats.at[t], st_s.at[t], st_r.at[t], t_dev(t)).wait_recv()

    def got_kv(s):
        remote(kvs.at[s], kvs.at[s], kv_s.at[s], kv_r.at[s], s_dev(s)).wait_recv()

    def relay_q(t, c):
        return remote(
            qd.at[t, c], qd.at[t, c], rq_s.at[t, c], qd_r.at[t, c], t_dev(near_t)
        )

    def relay_kv(s):
        return remote(kvs.at[s], kvs.at[s], rkv_s.at[s], kv_r.at[s], s_dev(near_s))

    def dq_copy(t):
        return remote(dq_out.at[t], dq_in.at[me_t], dq_s.at[t], dq_r.at[me_t], t_dev(t))

    def send_g(s, i):
        g_out[s, i] = dv[s].astype(BF16) if i else (dk[s] * scale).astype(BF16)
        remote(
            g_out.at[s, i], g_in.at[me_s, i], g_s.at[s, i], g_r.at[me_s, i], s_dev(s)
        ).start()

    tile(me_t, me_s)
    for s in far_s:
        got_kv(s)
        relay_kv(s).start()
    got_kv(near_s)
    tile(me_t, near_s)
    for c in range(2):
        for t in far_t:
            got_q(t, c)
            relay_q(t, c).start()
        if c == 0:
            for s in far_s:
                tile(me_t, s)
            for c2 in range(2):
                got_q(near_t, c2)
            got_stats(near_t)
    for s in [me_s, near_s] + far_s:
        tile(near_t, s)
    for t in far_t:
        got_stats(t)
        for s in [me_s, near_s] + far_s:
            tile(t, s)
    for s in diag_s:
        got_kv(s)
        for t in [near_t] + far_t + [me_t]:
            tile(t, s)
    dq_out[near_t] = (dq_acc[near_t] * scale).astype(BF16)
    dq_copy(near_t).start()
    for n, t in enumerate(diag_t):
        for c in range(2):
            got_q(t, c)
        got_stats(t)
        for s in far_s + diag_s + [near_s]:
            tile(t, s)
            if n == len(diag_t) - 1:
                send_g(s, 0)
        if n == len(diag_t) - 1:
            for s in far_s + diag_s + [near_s]:
                send_g(s, 1)
        tile(t, me_s)
        dq_out[t] = (dq_acc[t] * scale).astype(BF16)
        remote(dq_out.at[t], dq_via.at[t], dq_s.at[t], via_r.at[t], t_dev(near_t)).start()
    for t in far_t:
        remote(dq_out.at[t], dq_via.at[t], dq_s.at[t], via_r.at[t], t_dev(near_t)).wait_recv()
        dq_out[t] = (dq_acc[t] * scale + dq_via[t].astype(F32)).astype(BF16)
        dq_copy(t).start()

    def reduce_g(i):
        total = dv[me_s] if i else dk[me_s] * scale
        for s in s_peers:
            remote(
                g_in.at[s, i], g_in.at[s, i], g_s.at[s, i], g_r.at[s, i], s_dev(s)
            ).wait_recv()
            total += g_in[s, i].astype(F32)
        tp_own[i] = total.astype(BF16)
        for p in tp_peers:
            remote(
                tp_own.at[i], tp_in.at[tp, i], tp_s.at[p, i], tp_r.at[tp, i], tp_dev(p)
            ).start()
        tp_in[tp, i] = tp_own[i]

    def gather_g(i):
        for p in tp_peers:
            remote(
                tp_in.at[p, i], tp_in.at[p, i], tp_s.at[p, i], tp_r.at[p, i], tp_dev(p)
            ).wait_recv()
        for g in range(KV_HEADS):
            owners = [p for p in range(tp_n) if p * heads // per_key == g]
            half = tp_in[owners[0], i]
            if len(owners) > 1:
                total = half.astype(F32)
                for p in owners[1:]:
                    total += tp_in[p, i].astype(F32)
                half = total.astype(BF16)
            kv_ref[:, pl.ds((i * KV_HEADS + g) * HEAD_DIM, HEAD_DIM)] = half

    reduce_g(0)
    load.wait()
    gather_g(0)
    part = a2_own.shape[1]
    cut = a2_own.shape[2]
    key_half = kv_ref[:, 0 : KV_HEADS * HEAD_DIM]
    w_scale = 1.0 / math.sqrt(src_total)
    partial = dot_tn(key_half, src[...]) * w_scale
    for o in range(key_m):
        for i in range(key_n):
            low = (o * key_n + i) * part
            block = partial[low : low + part].astype(BF16)
            a_out[i, o] = block[:, :cut]
            b_out[o, i] = block[:, cut:]
    for i in i_peers:
        remote(a_out.at[i], a_in.at[me_i], a_s.at[i], a_r.at[me_i], i_dev(i)).start()
    for o in o_peers:
        remote(b_out.at[o], b_in.at[me_o], b_s.at[o], b_r.at[me_o], o_dev(o)).start()

    reduce_g(1)
    gather_g(1)
    dq_total = dq_acc[me_t] * scale
    for t in [near_t] + far_t:
        remote(dq_in.at[t], dq_in.at[t], dq_s.at[t], dq_r.at[t], t_dev(t)).wait_recv()
        dq_total += dq_in[t].astype(F32)
    for h in range(heads):
        low = h % per_chunk * rows
        dq_ref[:, h * HEAD_DIM : (h + 1) * HEAD_DIM] = dq_total[h // per_chunk, low : low + rows]

    total = b_out[me_o].astype(F32)
    for o in o_peers:
        remote(b_in.at[o], b_in.at[o], b_s.at[o], b_r.at[o], o_dev(o)).wait_recv()
        total += b_in[o].astype(F32)
    b2_own[...] = total
    b2_out[...] = total.astype(BF16)
    for i in i_peers:
        remote(b2_out.at[i], b2_in.at[me_i], b2_s.at[i], b2_r.at[me_i], i_dev(i)).start()
    total = a_out[me_i].astype(F32)
    for i in i_peers:
        remote(a_in.at[i], a_in.at[i], a_s.at[i], a_r.at[i], i_dev(i)).wait_recv()
        total += a_in[i].astype(F32)
    a2_own[...] = total
    a2_out[...] = total.astype(BF16)
    for o in o_peers:
        remote(a2_out.at[o], a2_in.at[me_o], a2_s.at[o], a2_r.at[me_o], o_dev(o)).start()
    total = b2_own[me_i]
    for i in i_peers:
        remote(b2_in.at[i], b2_in.at[i], b2_s.at[i], b2_r.at[i], i_dev(i)).wait_recv()
        total += b2_in[i].astype(F32)
    kg_ref[:, cut:] = total
    total = a2_own[me_o]
    for o in o_peers:
        remote(a2_in.at[o], a2_in.at[o], a2_s.at[o], a2_r.at[o], o_dev(o)).wait_recv()
        total += a2_in[o].astype(F32)
    kg_ref[:, :cut] = total

    for t in far_t + [near_t]:
        for c in range(2):
            remote(qd.at[t, c], qd.at[t, c], qd_s.at[t, c], qd_r.at[t, c], t_dev(t)).wait_send()
    for t in far_t:
        for c in range(2):
            relay_q(t, c).wait_send()
    for t in t_peers:
        remote(stats.at[t], stats.at[t], st_s.at[t], st_r.at[t], t_dev(t)).wait_send()
        remote(dq_out.at[t], dq_in.at[t], dq_s.at[t], dq_r.at[t], t_dev(t)).wait_send()
    for s in far_s + [near_s]:
        remote(kvs.at[s], kvs.at[s], kv_s.at[s], kv_r.at[s], s_dev(s)).wait_send()
    for s in far_s:
        relay_kv(s).wait_send()
    for s in s_peers:
        for i in range(2):
            remote(
                g_out.at[s, i], g_in.at[s, i], g_s.at[s, i], g_r.at[s, i], s_dev(s)
            ).wait_send()
    for i in i_peers:
        remote(a_out.at[i], a_in.at[i], a_s.at[i], a_r.at[i], i_dev(i)).wait_send()
        remote(b2_out.at[i], b2_in.at[i], b2_s.at[i], b2_r.at[i], i_dev(i)).wait_send()
    for o in o_peers:
        remote(b_out.at[o], b_in.at[o], b_s.at[o], b_r.at[o], o_dev(o)).wait_send()
        remote(a2_out.at[o], a2_in.at[o], a2_s.at[o], a2_r.at[o], o_dev(o)).wait_send()
    for p in tp_peers:
        for i in range(2):
            remote(
                tp_own.at[i], tp_in.at[p, i], tp_s.at[p, i], tp_r.at[p, i], tp_dev(p)
            ).wait_send()


def shards(
    tgt_n, src_n, tp_n,
    queries, attn_out, out_grad, row_lse, source, saved_keys, saved_values, key_weight, value_weight
):
    heads = row_lse.shape[1]
    rows, width = queries.shape
    src_rows, columns = source.shape
    kv_width = KV_HEADS * HEAD_DIM
    sp_n = tgt_n * src_n
    part = kv_width // sp_n
    key_n, key_m = src_n, tgt_n
    chunks = math.gcd(heads, 2)
    stacked = heads // chunks * rows
    cut = (2 * columns // 3 + 127) // 128 * 128
    rest = columns - cut
    dma = pltpu.SemaphoreType.DMA
    vmem = pl.BlockSpec(memory_space=pltpu.VMEM)
    scratch = [
        pltpu.VMEM((tgt_n, 2, rows, width), BF16),
        pltpu.VMEM((tgt_n, chunks, 8, stacked), F32),
        pltpu.VMEM((src_n, 2, src_rows, HEAD_DIM), BF16),
        pltpu.VMEM((src_n, src_rows, HEAD_DIM), F32),
        pltpu.VMEM((src_n, src_rows, HEAD_DIM), F32),
        pltpu.VMEM((tgt_n, chunks, stacked, HEAD_DIM), F32),
        pltpu.VMEM((tgt_n, chunks, stacked, HEAD_DIM), BF16),
        pltpu.VMEM((tgt_n, chunks, stacked, HEAD_DIM), BF16),
        pltpu.VMEM((tgt_n, chunks, stacked, HEAD_DIM), BF16),
        pltpu.VMEM((src_n, 2, src_rows, HEAD_DIM), BF16),
        pltpu.VMEM((src_n, 2, src_rows, HEAD_DIM), BF16),
        pltpu.VMEM((2, src_rows, HEAD_DIM), BF16),
        pltpu.VMEM((tp_n, 2, src_rows, HEAD_DIM), BF16),
        pltpu.VMEM((src_rows, columns), BF16),
        pltpu.VMEM((key_n, key_m, part, cut), BF16),
        pltpu.VMEM((key_n, key_m, part, cut), BF16),
        pltpu.VMEM((key_m, part, cut), F32),
        pltpu.VMEM((key_m, part, cut), BF16),
        pltpu.VMEM((key_m, part, cut), BF16),
        pltpu.VMEM((key_m, key_n, part, rest), BF16),
        pltpu.VMEM((key_m, key_n, part, rest), BF16),
        pltpu.VMEM((key_n, part, rest), F32),
        pltpu.VMEM((key_n, part, rest), BF16),
        pltpu.VMEM((key_n, part, rest), BF16),
        dma,
    ]
    for shape in (
        (tgt_n, 2), (tgt_n, 2), (tgt_n, 2), (tgt_n,), (tgt_n,),
        (src_n,), (src_n,), (src_n,), (tgt_n,), (tgt_n,), (tgt_n,), (src_n, 2), (src_n, 2),
        (tp_n, 2), (tp_n, 2), (key_n,), (key_n,), (key_m,), (key_m,),
        (key_m,), (key_m,), (key_n,), (key_n,),
    ):
        scratch.append(dma(shape))
    query_grad, kv_half, key_grad = pl.pallas_call(
        functools.partial(kernel, tgt_n, src_n, key_n, tp_n, src_rows * sp_n),
        out_shape=(
            jax.ShapeDtypeStruct((rows, width), F32),
            jax.ShapeDtypeStruct((src_rows, 2 * kv_width), BF16),
            jax.ShapeDtypeStruct((part, columns), F32),
        ),
        in_specs=[vmem] * 6 + [pl.BlockSpec(memory_space=pl.ANY)],
        out_specs=(vmem, vmem, vmem),
        scratch_shapes=scratch,
        compiler_params=pltpu.CompilerParams(
            collective_id=0, has_side_effects=True, vmem_limit_bytes=60 * 2**20
        ),
        name="attention_grads",
    )(queries, attn_out, out_grad, row_lse.T, saved_keys, saved_values, source)
    source_grad = dot_nt(kv_half[:, :kv_width], key_weight) + dot_nt(
        kv_half[:, kv_width:], value_weight
    )
    return (query_grad, source_grad, key_grad)


def solution(mesh):
    sp_n, tp_n = mesh.shape["sp"], mesh.shape["tp"]
    src_n = 2 ** (int(math.log2(sp_n)) // 2)
    in_specs = (
        P("sp", "tp"),
        P("sp", "tp"),
        P("sp", "tp"),
        P("sp", "tp"),
        P("sp", "tp"),
        P("sp", None),
        P("sp", None),
        P("tp", None),
        P("tp", None),
    )
    out_specs = (P("sp", "tp"), P("sp", "tp"), P("sp", "tp"))
    return jax.shard_map(
        functools.partial(shards, sp_n // src_n, src_n, tp_n),
        mesh=mesh, in_specs=in_specs, out_specs=out_specs, check_vma=False,
    )
```

```python
import functools
import math

import jax
import jax.numpy as jnp
from jax import lax
from jax.experimental import pallas as pl
from jax.experimental.pallas import tpu as pltpu
from jax.sharding import PartitionSpec as P

HEADS = 8
KV_HEADS = 2
HEAD_DIM = 128
LOG2E = 1.0 / math.log(2.0)
MESH = pl.DeviceIdType.MESH
F32 = jnp.float32
BF16 = jnp.bfloat16


def dot_nt(left, right, precision=None):
    return lax.dot_general(
        left, right, (((1,), (1,)), ((), ())), preferred_element_type=F32, precision=precision
    )


def dot_tn(left, right):
    return lax.dot_general(left, right, (((0,), (0,)), ((), ())), preferred_element_type=F32)


def dot_nn(left, right):
    return jnp.dot(left, right, preferred_element_type=F32)


def kernel(
    tgt_n, src_n, key_n, tp_n, src_total,
    q_ref, o_ref, d_ref, lse_ref, key_ref, value_ref, source_ref,
    dq_ref, kv_ref, kg_ref,
    qd, stats, kvs, dk, dv, dq_acc, dq_out, dq_in, dq_via, g_out, g_in, tp_own, tp_in,
    src, a_out, a_in, a2_own, a2_out, a2_in, b_out, b_in, b2_own, b2_out, b2_in,
    copy_sem, qd_s, qd_r, rq_s, st_s, st_r, kv_s, kv_r, rkv_s, dq_s, dq_r, via_r, g_s, g_r, tp_s, tp_r,
    a_s, a_r, a2_s, a2_r, b_s, b_r, b2_s, b2_r,
):
    sp = lax.axis_index("sp")
    tp = lax.axis_index("tp")
    sp_n = tgt_n * src_n
    t_hi, t_lo = sp // (2 * src_n), sp % 2
    me_t = t_hi * 2 + t_lo
    me_s = (sp // 2) % src_n
    s_hi, s_lo = me_s // 2, me_s % 2
    near_t, near_s = t_hi * 2 + 1 - t_lo, s_hi * 2 + 1 - s_lo
    t_his = [lax.rem(t_hi + k, tgt_n // 2) for k in range(1, tgt_n // 2)]
    s_his = [lax.rem(s_hi + k, src_n // 2) for k in range(1, src_n // 2)]
    far_t = [hi * 2 + t_lo for hi in t_his]
    diag_t = [hi * 2 + 1 - t_lo for hi in t_his]
    far_s = [hi * 2 + s_lo for hi in s_his]
    diag_s = [hi * 2 + 1 - s_lo for hi in s_his]
    t_peers = far_t + [near_t] + diag_t
    s_peers = far_s + [near_s] + diag_s
    key_m = sp_n // key_n
    me_o, me_i = sp // key_n, sp % key_n
    o_peers = [lax.rem(me_o + k, key_m) for k in range(1, key_m)]
    i_peers = [lax.rem(me_i + k, key_n) for k in range(1, key_n)]
    tp_peers = [lax.rem(tp + k, tp_n) for k in range(1, tp_n)]
    rows = q_ref.shape[0]
    heads = q_ref.shape[1] // HEAD_DIM
    chunks = stats.shape[1]
    per_chunk = heads // chunks
    src_rows = key_ref.shape[0]
    per_key = HEADS // KV_HEADS
    scale = 1.0 / math.sqrt(HEAD_DIM)
    kv_col = pl.multiple_of(tp * heads // per_key * HEAD_DIM, HEAD_DIM)

    def t_dev(t):
        return {"sp": t // 2 * (2 * src_n) + me_s * 2 + t % 2, "tp": tp}

    def s_dev(s):
        return {"sp": t_hi * (2 * src_n) + s * 2 + t_lo, "tp": tp}

    def o_dev(o):
        return {"sp": o * key_n + me_i, "tp": tp}

    def i_dev(i):
        return {"sp": me_o * key_n + i, "tp": tp}

    def tp_dev(p):
        return {"sp": sp, "tp": p}

    def remote(source, target, send, recv, device):
        return pltpu.make_async_remote_copy(
            src_ref=source, dst_ref=target, send_sem=send, recv_sem=recv,
            device_id=device, device_id_type=MESH,
        )

    load = pltpu.make_async_copy(source_ref, src, copy_sem)
    load.start()
    barrier = pltpu.get_barrier_semaphore()
    for k in range(1, sp_n):
        pl.semaphore_signal(
            barrier, inc=1, device_id={"sp": lax.rem(sp + k, sp_n), "tp": tp}, device_id_type=MESH
        )
    for p in tp_peers:
        pl.semaphore_signal(barrier, inc=1, device_id=tp_dev(p), device_id_type=MESH)
    ones = jnp.ones((8, HEAD_DIM), F32)
    for h in range(heads):
        cols = pl.ds(h * HEAD_DIM, HEAD_DIM)
        c, span = h // per_chunk, pl.ds(h % per_chunk * rows, rows)
        prod = d_ref[:, cols].astype(F32) * o_ref[:, cols].astype(F32)
        delta = dot_nt(ones, prod, lax.Precision.HIGHEST)
        stats[me_t, c, 0:1, span] = lse_ref[h : h + 1, :] * LOG2E
        stats[me_t, c, 1:2, span] = delta[0:1, :]
    kvs[me_s, 0] = key_ref[:, pl.ds(kv_col, HEAD_DIM)]
    kvs[me_s, 1] = value_ref[:, pl.ds(kv_col, HEAD_DIM)]
    qd[me_t, 0] = q_ref[...]
    qd[me_t, 1] = d_ref[...]
    dk[...] = jnp.zeros_like(dk)
    dv[...] = jnp.zeros_like(dv)
    dq_acc[...] = jnp.zeros_like(dq_acc)
    pl.semaphore_wait(barrier, sp_n + tp_n - 2)

    def send_q(t):
        for i, ref in enumerate((q_ref, d_ref)):
            remote(ref, qd.at[me_t, i], qd_s.at[t, i], qd_r.at[me_t, i], t_dev(t)).start()

    for s in far_s + [near_s]:
        remote(kvs.at[me_s], kvs.at[me_s], kv_s.at[s], kv_r.at[me_s], s_dev(s)).start()
    for t in far_t + [near_t]:
        send_q(t)

    for t in t_peers:
        remote(stats.at[me_t], stats.at[me_t], st_s.at[t], st_r.at[me_t], t_dev(t)).start()

    def stack(t, i, c):
        low = c * per_chunk
        return jnp.concatenate(
            [
                qd[t, i, :, pl.ds(pl.multiple_of((low + h) * HEAD_DIM, HEAD_DIM), HEAD_DIM)]
                for h in range(per_chunk)
            ],
            axis=0,
        )

    def tile(t, s):
        def body(c, carry):
            q, d = stack(t, 0, c), stack(t, 1, c)
            k, v = kvs[s, 0], kvs[s, 1]
            scores = dot_nt(k, q)
            probs = jnp.exp2(scores * (scale * LOG2E) - stats[t, c, 0:1, :])
            dprobs = dot_nt(v, d)
            dscores = (probs * (dprobs - stats[t, c, 1:2, :])).astype(BF16)
            dv[s] += dot_nn(probs.astype(BF16), d)
            dk[s] += dot_nn(dscores, q)
            dq_acc[t, c] += dot_tn(dscores, k)
            return carry

        lax.fori_loop(0, chunks, body, 0)

    def got_q(t, c):
        remote(qd.at[t, c], qd.at[t, c], qd_s.at[t, c], qd_r.at[t, c], t_dev(t)).wait_recv()

    def got_stats(t):
        remote(stats.at[t], stats.at[t], st_s.at[t], st_r.at[t], t_dev(t)).wait_recv()

    def got_kv(s):
        remote(kvs.at[s], kvs.at[s], kv_s.at[s], kv_r.at[s], s_dev(s)).wait_recv()

    def relay_q(t, c):
        return remote(
            qd.at[t, c], qd.at[t, c], rq_s.at[t, c], qd_r.at[t, c], t_dev(near_t)
        )

    def relay_kv(s):
        return remote(kvs.at[s], kvs.at[s], rkv_s.at[s], kv_r.at[s], s_dev(near_s))

    def dq_copy(t):
        return remote(dq_out.at[t], dq_in.at[me_t], dq_s.at[t], dq_r.at[me_t], t_dev(t))

    def send_g(s, i):
        g_out[s, i] = dv[s].astype(BF16) if i else (dk[s] * scale).astype(BF16)
        remote(
            g_out.at[s, i], g_in.at[me_s, i], g_s.at[s, i], g_r.at[me_s, i], s_dev(s)
        ).start()

    tile(me_t, me_s)
    for s in far_s:
        got_kv(s)
        relay_kv(s).start()
    got_kv(near_s)
    tile(me_t, near_s)
    for c in range(2):
        for t in far_t:
            got_q(t, c)
            relay_q(t, c).start()
        if c == 0:
            for s in far_s:
                tile(me_t, s)
            for c2 in range(2):
                got_q(near_t, c2)
            got_stats(near_t)
    for s in [me_s, near_s] + far_s:
        tile(near_t, s)
    for t in far_t:
        got_stats(t)
        for s in [me_s, near_s] + far_s:
            tile(t, s)
    for s in diag_s:
        got_kv(s)
        for t in [near_t] + far_t + [me_t]:
            tile(t, s)
    dq_out[near_t] = (dq_acc[near_t] * scale).astype(BF16)
    dq_copy(near_t).start()
    for n, t in enumerate(diag_t):
        for c in range(2):
            got_q(t, c)
        got_stats(t)
        for s in far_s + diag_s + [near_s]:
            tile(t, s)
            if n == len(diag_t) - 1:
                send_g(s, 0)
        if n == len(diag_t) - 1:
            for s in far_s + diag_s + [near_s]:
                send_g(s, 1)
        tile(t, me_s)
        dq_out[t] = (dq_acc[t] * scale).astype(BF16)
        remote(dq_out.at[t], dq_via.at[t], dq_s.at[t], via_r.at[t], t_dev(near_t)).start()
    for t in far_t:
        remote(dq_out.at[t], dq_via.at[t], dq_s.at[t], via_r.at[t], t_dev(near_t)).wait_recv()
        dq_out[t] = (dq_acc[t] * scale + dq_via[t].astype(F32)).astype(BF16)
        dq_copy(t).start()

    def reduce_g(i):
        total = dv[me_s] if i else dk[me_s] * scale
        for s in s_peers:
            remote(
                g_in.at[s, i], g_in.at[s, i], g_s.at[s, i], g_r.at[s, i], s_dev(s)
            ).wait_recv()
            total += g_in[s, i].astype(F32)
        tp_own[i] = total.astype(BF16)
        for p in tp_peers:
            remote(
                tp_own.at[i], tp_in.at[tp, i], tp_s.at[p, i], tp_r.at[tp, i], tp_dev(p)
            ).start()
        tp_in[tp, i] = tp_own[i]

    def gather_g(i):
        for p in tp_peers:
            remote(
                tp_in.at[p, i], tp_in.at[p, i], tp_s.at[p, i], tp_r.at[p, i], tp_dev(p)
            ).wait_recv()
        for g in range(KV_HEADS):
            owners = [p for p in range(tp_n) if p * heads // per_key == g]
            half = tp_in[owners[0], i]
            if len(owners) > 1:
                total = half.astype(F32)
                for p in owners[1:]:
                    total += tp_in[p, i].astype(F32)
                half = total.astype(BF16)
            kv_ref[:, pl.ds((i * KV_HEADS + g) * HEAD_DIM, HEAD_DIM)] = half

    reduce_g(0)
    load.wait()
    gather_g(0)
    part = a2_own.shape[1]
    cut = a2_own.shape[2]
    key_half = kv_ref[:, 0 : KV_HEADS * HEAD_DIM]
    w_scale = 1.0 / math.sqrt(src_total)
    partial = dot_tn(key_half, src[...]) * w_scale
    for o in range(key_m):
        for i in range(key_n):
            low = (o * key_n + i) * part
            block = partial[low : low + part].astype(BF16)
            a_out[i, o] = block[:, :cut]
            b_out[o, i] = block[:, cut:]
    for i in i_peers:
        remote(a_out.at[i], a_in.at[me_i], a_s.at[i], a_r.at[me_i], i_dev(i)).start()
    for o in o_peers:
        remote(b_out.at[o], b_in.at[me_o], b_s.at[o], b_r.at[me_o], o_dev(o)).start()

    reduce_g(1)
    gather_g(1)
    dq_total = dq_acc[me_t] * scale
    for t in [near_t] + far_t:
        remote(dq_in.at[t], dq_in.at[t], dq_s.at[t], dq_r.at[t], t_dev(t)).wait_recv()
        dq_total += dq_in[t].astype(F32)
    for h in range(heads):
        low = h % per_chunk * rows
        dq_ref[:, h * HEAD_DIM : (h + 1) * HEAD_DIM] = dq_total[h // per_chunk, low : low + rows]

    total = b_out[me_o].astype(F32)
    for o in o_peers:
        remote(b_in.at[o], b_in.at[o], b_s.at[o], b_r.at[o], o_dev(o)).wait_recv()
        total += b_in[o].astype(F32)
    b2_own[...] = total
    b2_out[...] = total.astype(BF16)
    for i in i_peers:
        remote(b2_out.at[i], b2_in.at[me_i], b2_s.at[i], b2_r.at[me_i], i_dev(i)).start()
    total = a_out[me_i].astype(F32)
    for i in i_peers:
        remote(a_in.at[i], a_in.at[i], a_s.at[i], a_r.at[i], i_dev(i)).wait_recv()
        total += a_in[i].astype(F32)
    a2_own[...] = total
    a2_out[...] = total.astype(BF16)
    for o in o_peers:
        remote(a2_out.at[o], a2_in.at[me_o], a2_s.at[o], a2_r.at[me_o], o_dev(o)).start()
    total = b2_own[me_i]
    for i in i_peers:
        remote(b2_in.at[i], b2_in.at[i], b2_s.at[i], b2_r.at[i], i_dev(i)).wait_recv()
        total += b2_in[i].astype(F32)
    kg_ref[:, cut:] = total
    total = a2_own[me_o]
    for o in o_peers:
        remote(a2_in.at[o], a2_in.at[o], a2_s.at[o], a2_r.at[o], o_dev(o)).wait_recv()
        total += a2_in[o].astype(F32)
    kg_ref[:, :cut] = total

    for t in far_t + [near_t]:
        for c in range(2):
            remote(qd.at[t, c], qd.at[t, c], qd_s.at[t, c], qd_r.at[t, c], t_dev(t)).wait_send()
    for t in far_t:
        for c in range(2):
            relay_q(t, c).wait_send()
    for t in t_peers:
        remote(stats.at[t], stats.at[t], st_s.at[t], st_r.at[t], t_dev(t)).wait_send()
        remote(dq_out.at[t], dq_in.at[t], dq_s.at[t], dq_r.at[t], t_dev(t)).wait_send()
    for s in far_s + [near_s]:
        remote(kvs.at[s], kvs.at[s], kv_s.at[s], kv_r.at[s], s_dev(s)).wait_send()
    for s in far_s:
        relay_kv(s).wait_send()
    for s in s_peers:
        for i in range(2):
            remote(
                g_out.at[s, i], g_in.at[s, i], g_s.at[s, i], g_r.at[s, i], s_dev(s)
            ).wait_send()
    for i in i_peers:
        remote(a_out.at[i], a_in.at[i], a_s.at[i], a_r.at[i], i_dev(i)).wait_send()
        remote(b2_out.at[i], b2_in.at[i], b2_s.at[i], b2_r.at[i], i_dev(i)).wait_send()
    for o in o_peers:
        remote(b_out.at[o], b_in.at[o], b_s.at[o], b_r.at[o], o_dev(o)).wait_send()
        remote(a2_out.at[o], a2_in.at[o], a2_s.at[o], a2_r.at[o], o_dev(o)).wait_send()
    for p in tp_peers:
        for i in range(2):
            remote(
                tp_own.at[i], tp_in.at[p, i], tp_s.at[p, i], tp_r.at[p, i], tp_dev(p)
            ).wait_send()


def finish_kernel(
    kv_hbm, kw_hbm, vw_hbm, dq_hbm, kg_hbm, out_ref, dq_out, kg_out,
    kv, kw, vw, dq, kg, buf, in_sems, w_sems, out_sems, pass_sems,
):
    half = kw.shape[1]
    width = buf.shape[2]
    count = buf.shape[0]
    load = pltpu.make_async_copy(kv_hbm, kv, in_sems.at[0])
    load.start()
    loads = []
    for n in range(count):
        cols = pl.ds(n * width, width)
        loads.append(
            [
                pltpu.make_async_copy(ref.at[cols], to.at[cols], w_sems.at[n, i])
                for i, (ref, to) in enumerate(((kw_hbm, kw), (vw_hbm, vw)))
            ]
        )
        for copy in loads[n]:
            copy.start()
    dq_in = pltpu.make_async_copy(dq_hbm, dq, in_sems.at[1])
    kg_in = pltpu.make_async_copy(kg_hbm, kg, in_sems.at[2])
    dq_in.start()
    kg_in.start()
    load.wait()
    copies = []
    for n in range(count):
        cols = slice(n * width, (n + 1) * width)
        for copy in loads[n]:
            copy.wait()
        buf[n] = dot_nt(kv[:, :half], kw[cols]) + dot_nt(kv[:, half:], vw[cols])
        copies.append(
            pltpu.make_async_copy(
                buf.at[n], out_ref.at[:, pl.ds(n * width, width)], out_sems.at[n]
            )
        )
        copies[n].start()
    dq_in.wait()
    copies.append(pltpu.make_async_copy(dq, dq_out, pass_sems.at[0]))
    copies[-1].start()
    kg_in.wait()
    copies.append(pltpu.make_async_copy(kg, kg_out, pass_sems.at[1]))
    copies[-1].start()
    for copy in copies:
        copy.wait()


def shards(
    tgt_n, src_n, tp_n,
    queries, attn_out, out_grad, row_lse, source, saved_keys, saved_values, key_weight, value_weight
):
    heads = row_lse.shape[1]
    rows, width = queries.shape
    src_rows, columns = source.shape
    kv_width = KV_HEADS * HEAD_DIM
    sp_n = tgt_n * src_n
    part = kv_width // sp_n
    key_n, key_m = src_n, tgt_n
    chunks = math.gcd(heads, 2)
    stacked = heads // chunks * rows
    cut = (2 * columns // 3 + 127) // 128 * 128
    rest = columns - cut
    dma = pltpu.SemaphoreType.DMA
    vmem = pl.BlockSpec(memory_space=pltpu.VMEM)
    scratch = [
        pltpu.VMEM((tgt_n, 2, rows, width), BF16),
        pltpu.VMEM((tgt_n, chunks, 8, stacked), F32),
        pltpu.VMEM((src_n, 2, src_rows, HEAD_DIM), BF16),
        pltpu.VMEM((src_n, src_rows, HEAD_DIM), F32),
        pltpu.VMEM((src_n, src_rows, HEAD_DIM), F32),
        pltpu.VMEM((tgt_n, chunks, stacked, HEAD_DIM), F32),
        pltpu.VMEM((tgt_n, chunks, stacked, HEAD_DIM), BF16),
        pltpu.VMEM((tgt_n, chunks, stacked, HEAD_DIM), BF16),
        pltpu.VMEM((tgt_n, chunks, stacked, HEAD_DIM), BF16),
        pltpu.VMEM((src_n, 2, src_rows, HEAD_DIM), BF16),
        pltpu.VMEM((src_n, 2, src_rows, HEAD_DIM), BF16),
        pltpu.VMEM((2, src_rows, HEAD_DIM), BF16),
        pltpu.VMEM((tp_n, 2, src_rows, HEAD_DIM), BF16),
        pltpu.VMEM((src_rows, columns), BF16),
        pltpu.VMEM((key_n, key_m, part, cut), BF16),
        pltpu.VMEM((key_n, key_m, part, cut), BF16),
        pltpu.VMEM((key_m, part, cut), F32),
        pltpu.VMEM((key_m, part, cut), BF16),
        pltpu.VMEM((key_m, part, cut), BF16),
        pltpu.VMEM((key_m, key_n, part, rest), BF16),
        pltpu.VMEM((key_m, key_n, part, rest), BF16),
        pltpu.VMEM((key_n, part, rest), F32),
        pltpu.VMEM((key_n, part, rest), BF16),
        pltpu.VMEM((key_n, part, rest), BF16),
        dma,
    ]
    for shape in (
        (tgt_n, 2), (tgt_n, 2), (tgt_n, 2), (tgt_n,), (tgt_n,),
        (src_n,), (src_n,), (src_n,), (tgt_n,), (tgt_n,), (tgt_n,), (src_n, 2), (src_n, 2),
        (tp_n, 2), (tp_n, 2), (key_n,), (key_n,), (key_m,), (key_m,),
        (key_m,), (key_m,), (key_n,), (key_n,),
    ):
        scratch.append(dma(shape))
    query_grad, kv_half, key_grad = pl.pallas_call(
        functools.partial(kernel, tgt_n, src_n, key_n, tp_n, src_rows * sp_n),
        out_shape=(
            jax.ShapeDtypeStruct((rows, width), F32),
            jax.ShapeDtypeStruct((src_rows, 2 * kv_width), BF16),
            jax.ShapeDtypeStruct((part, columns), F32),
        ),
        in_specs=[vmem] * 6 + [pl.BlockSpec(memory_space=pl.ANY)],
        out_specs=(vmem, vmem, vmem),
        scratch_shapes=scratch,
        compiler_params=pltpu.CompilerParams(
            collective_id=0, has_side_effects=True, vmem_limit_bytes=60 * 2**20
        ),
        name="attention_grads",
    )(queries, attn_out, out_grad, row_lse.T, saved_keys, saved_values, source)
    local_columns = key_weight.shape[0]
    blocks = local_columns // math.gcd(local_columns, 256)
    hbm = pl.BlockSpec(memory_space=pl.ANY)
    source_grad, query_grad, key_grad = pl.pallas_call(
        finish_kernel,
        out_shape=(
            jax.ShapeDtypeStruct((src_rows, local_columns), F32),
            jax.ShapeDtypeStruct((rows, width), F32),
            jax.ShapeDtypeStruct((part, columns), F32),
        ),
        in_specs=[hbm] * 5,
        out_specs=(hbm, hbm, hbm),
        scratch_shapes=[
            pltpu.VMEM((src_rows, 2 * kv_width), BF16),
            pltpu.VMEM((local_columns, kv_width), BF16),
            pltpu.VMEM((local_columns, kv_width), BF16),
            pltpu.VMEM((rows, width), F32),
            pltpu.VMEM((part, columns), F32),
            pltpu.VMEM((blocks, src_rows, local_columns // blocks), F32),
            dma((3,)),
            dma((blocks, 2)),
            dma((blocks,)),
            dma((2,)),
        ],
        compiler_params=pltpu.CompilerParams(vmem_limit_bytes=60 * 2**20),
        name="source_grads",
    )(kv_half, key_weight, value_weight, query_grad, key_grad)
    return (query_grad, source_grad, key_grad)


def solution(mesh):
    sp_n, tp_n = mesh.shape["sp"], mesh.shape["tp"]
    src_n = 2 ** (int(math.log2(sp_n)) // 2)
    in_specs = (
        P("sp", "tp"),
        P("sp", "tp"),
        P("sp", "tp"),
        P("sp", "tp"),
        P("sp", "tp"),
        P("sp", None),
        P("sp", None),
        P("tp", None),
        P("tp", None),
    )
    out_specs = (P("sp", "tp"), P("sp", "tp"), P("sp", "tp"))
    return jax.shard_map(
        functools.partial(shards, sp_n // src_n, src_n, tp_n),
        mesh=mesh, in_specs=in_specs, out_specs=out_specs, check_vma=False,
    )
```
